32 devices in a mesh: grp: 2 (over y), fs: 4 (over z), tp: 4 (over x, core).
Axes of the slice: x: 2, y: 2, z: 4, core: 2. Of those that a mesh axis runs over, the one named last changes fastest.
Arguments:
- layer_input: bfloat16 [3072, 2048], P(('grp', 'fs'), 'tp'), parts along dimension 0, may hold values from -6 to 6
- first_gain: bfloat16 [1, 2048], P(None, 'tp'), may hold values from 0.099609375 to 1.8984375
- ffn_gate_w: bfloat16 [2048, 6144], P('fs', 'tp'), may hold values from -0.125 to 0.125
- ffn_up_w: bfloat16 [2048, 6144], P('fs', 'tp'), may hold values from -0.125 to 0.125
- ffn_down_w: bfloat16 [6144, 2048], P('tp', 'fs'), may hold values from -0.078125 to 0.078125
- mixer_gain: bfloat16 [1, 2048], P(None, 'tp'), may hold values from 0.099609375 to 1.8984375
- pool_in_w: bfloat16 [2048, 1024], P('fs', 'tp'), may hold values from -0.125 to 0.125
- mixer_gate_w: bfloat16 [2048, 2048], P('fs', 'tp'), may hold values from -0.125 to 0.125
- group_mix_w: bfloat16 [8, 128, 128], P('tp'), may hold values from -0.5 to 0.5
- pool_scale: float32 [1, 1024], P(None, 'tp'), may hold values from 0.1 to 1.9
- mixer_out_w: bfloat16 [1024, 2048], P('tp', 'fs'), may hold values from -0.1875 to 0.1875
- second_gain: bfloat16 [1, 2048], P(None, 'tp'), may hold values from 0.099609375 to 1.8984375
Outputs:
- layer_output: bfloat16 [3072, 2048], P(('grp', 'fs'), 'tp'), parts along dimension 0
The draws below stay inside these ranges and needn't reach their ends.
There are 2 independent parts, one for each index of `grp`. The reference program is written for one: setup_inputs(seed, part) draws one part's arguments, and reference() takes and returns one part's arrays. A program takes and returns all parts, laid end to end along the dimension named above; an argument that names none is the same for every part. Nothing has to cross between parts.
All inputs are finite; a program needn't handle non-finite values.
Results may differ from the reference program's by a relative error of at most 0.015.
Values may be sent and summed in bfloat16 or wider, within the bound.
A program may use at most 64 MiB of HBM per device.

```python
import jax
import jax.numpy as jnp
from jax import lax

D = 2048
FF = 6144
BW = 1024
GW = 128
GROUPS = 8
TOK_DEV = 384
TOKENS = 1536
N_FS = 4
N_TP = 4


def steps_of(key, dims, split, low, top_value):
    factor_of = 1.0
    for position, shards_of in split:
        draws = jax.random.uniform(jax.random.fold_in(jax.random.fold_in(key, 6), position), (shards_of,), jnp.float32, low / len(split), top_value / len(split))
        factor_of = factor_of * jnp.repeat(jnp.exp(draws), dims[position] // shards_of).reshape((-1,) + (1,) * (len(dims) - 1 - position))
    return factor_of


def noise(rng, extent, scale, bound, shards=(), kind=jnp.bfloat16):
    drawn = jax.random.normal(rng, extent, jnp.float32) * scale
    if len(shards) > 0:
        drawn = steps_of(rng, extent, shards, -0.22, 0.18) * drawn
    return jnp.clip(drawn, min=-bound, max=bound).astype(kind)


def setup_inputs(seed: int = 0, part: int = 0) -> dict:
    splits = jax.random.split(jax.random.key(seed), 13)
    part_keys = jax.random.split(jax.random.fold_in(splits[12], part), 13)
    layer_input = noise(part_keys[0], (TOKENS, D), 1.0, 6.0, ((0, 4), (1, 4)))
    first_gain = jnp.clip(1.0 + 0.18 * jax.random.normal(splits[1], (1, D), jnp.float32), 0.099609375, 1.8984375).astype(jnp.bfloat16)
    ffn_gate_w = noise(splits[2], (D, FF), D ** -0.5, 0.125, ((0, 4), (1, 4)))
    ffn_up_w = noise(splits[3], (D, FF), D ** -0.5, 0.125, ((0, 4), (1, 4)))
    ffn_down_w = noise(splits[4], (FF, D), FF ** -0.5, 0.078125, ((0, 4), (1, 4)))
    mixer_gain = jnp.clip(1.0 + 0.18 * jax.random.normal(splits[5], (1, D), jnp.float32), 0.099609375, 1.8984375).astype(jnp.bfloat16)
    pool_in_w = noise(splits[6], (D, BW), D ** -0.5, 0.125, ((0, 4), (1, 4)))
    mixer_gate_w = noise(splits[7], (D, D), D ** -0.5, 0.125, ((0, 4), (1, 4)))
    group_mix_w = noise(splits[8], (GROUPS, GW, GW), GW ** -0.5, 0.5, ((0, 4),))
    pool_scale = jnp.clip(1.0 + 0.18 * jax.random.normal(splits[9], (1, BW), jnp.float32), 0.1, 1.9)
    mixer_out_w = noise(splits[10], (BW, D), BW ** -0.5, 0.1875, ((0, 4), (1, 4)))
    second_gain = jnp.clip(1.0 + 0.18 * jax.random.normal(splits[11], (1, D), jnp.float32), 0.099609375, 1.8984375).astype(jnp.bfloat16)
    return dict(layer_input=layer_input, first_gain=first_gain, ffn_gate_w=ffn_gate_w, ffn_up_w=ffn_up_w, ffn_down_w=ffn_down_w, mixer_gain=mixer_gain, pool_in_w=pool_in_w, mixer_gate_w=mixer_gate_w, group_mix_w=group_mix_w, pool_scale=pool_scale, mixer_out_w=mixer_out_w, second_gain=second_gain)


def norm_rows(values, gain):
    widened = values.astype(jnp.float32)
    scaled = (widened * gain.astype(jnp.float32)).astype(jnp.bfloat16)
    factor = lax.rsqrt(lax.optimization_barrier(jnp.mean(widened * widened, axis=1, keepdims=True)) + 1e-06)
    return (scaled, factor)

def block_sum(left, right):
    width = left.shape[1] // N_TP
    total = jnp.zeros((left.shape[0], right.shape[1]), jnp.float32)
    for block in range(N_TP):
        partial_value = jnp.dot(left[:, block * width:(block + 1) * width], right[block * width:(block + 1) * width], preferred_element_type=jnp.float32)
        rounded = lax.optimization_barrier(partial_value.astype(jnp.bfloat16))
        total = total + rounded.astype(jnp.float32)
    return total

def feed_forward(values, gain, ffn_gate_w, ffn_up_w, ffn_down_w):
    scaled, factor = norm_rows(values, gain)
    gate_pre = factor * jnp.dot(scaled, ffn_gate_w, preferred_element_type=jnp.float32)
    up_pre = factor * jnp.dot(scaled, ffn_up_w, preferred_element_type=jnp.float32)
    hidden = (jax.nn.silu(gate_pre) * up_pre).astype(jnp.bfloat16)
    return block_sum(hidden, ffn_down_w)

def reference(layer_input, first_gain, ffn_gate_w, ffn_up_w, ffn_down_w, mixer_gain, pool_in_w, mixer_gate_w, group_mix_w, pool_scale, mixer_out_w, second_gain):
    first = (layer_input.astype(jnp.float32) + 0.5 * feed_forward(layer_input, first_gain, ffn_gate_w, ffn_up_w, ffn_down_w)).astype(jnp.bfloat16)
    scaled, factor = norm_rows(first, mixer_gain)
    pool_pre = (factor * jnp.dot(scaled, pool_in_w, preferred_element_type=jnp.float32)).astype(jnp.bfloat16)
    gate_logit = factor * jnp.dot(scaled, mixer_gate_w, preferred_element_type=jnp.float32)
    values = pool_pre.astype(jnp.float32).reshape(N_FS, TOK_DEV, GROUPS, GW)
    running = jnp.cumsum(values, axis=1)
    positions = jnp.arange(TOK_DEV, dtype=jnp.int32)
    windows = 2 ** (1 + jnp.arange(GROUPS, dtype=jnp.int32) % 4)
    chosen = jnp.zeros_like(values)
    for span in (2, 4, 8, 16):
        lagged = jnp.pad(running, ((0, 0), (span, 0), (0, 0), (0, 0)))[:, :TOK_DEV]
        counts = jnp.minimum(positions + 1, span).astype(jnp.float32)[None, :, None, None]
        means = (running - lagged) / counts
        chosen = jnp.where((windows == span)[None, None, :, None], means, chosen)
    trail = (chosen - values).astype(jnp.bfloat16)
    mixed = jnp.einsum('ntgc,gcd->ntgd', trail.astype(jnp.float32), group_mix_w.astype(jnp.float32))
    pooled = (mixed.reshape(TOKENS, BW) * pool_scale).astype(jnp.bfloat16)
    lifted = block_sum(pooled, mixer_out_w)
    second = (first.astype(jnp.float32) + jax.nn.sigmoid(gate_logit) * lifted).astype(jnp.bfloat16)
    result = second.astype(jnp.float32) + 0.5 * feed_forward(second, second_gain, ffn_gate_w, ffn_up_w, ffn_down_w)
    return result.astype(jnp.bfloat16)
```

```python
import functools

import jax
import jax.numpy as jnp
from jax import lax
from jax.experimental import pallas as pl
from jax.experimental.pallas import tpu as pltpu
from jax.sharding import PartitionSpec as P

MESH = pl.DeviceIdType.MESH
F32 = jnp.float32
BF16 = jnp.bfloat16
GAIN_ROWS = 16


def ceil_pieces(rows, wanted):
    while rows % (wanted * 16) != 0:
        wanted -= 1
    return wanted


def layer_kernel(
    sizes,
    payload,
    gate_w,
    up_w,
    down_w,
    pool_w,
    mgate_w,
    mout_w,
    mix_w,
    scale_w,
    out,
    gate_all,
    up_all,
    down_all,
    pool_all,
    mgate_all,
    mout_all,
    input_all,
    value_all,
    scaled,
    factor,
    hidden,
    pooled,
    logit,
    parts,
    sums,
    local_sem,
    z_recv,
    y_recv,
    up_sem,
    low_sem,
    y_sem,
    x_send,
    x_recv,
    s_send,
    s_recv,
):
    grps, planes, tps, piece_counts = sizes
    g = lax.axis_index("grp")
    f = lax.axis_index("fs")
    tp = lax.axis_index("tp")
    rows, width = out.shape
    chips = tps // 2
    chip, core = tp // 2, tp % 2
    peers = [
        ((chip + i) % chips) * 2 + (core + b) % 2 for i in range(1, chips) for b in range(2)
    ] + [chip * 2 + (core + 1) % 2]
    other_grps = [(g + d) % grps for d in range(1, grps)]

    barrier = pltpu.get_barrier_semaphore()
    for peer in peers:
        pl.semaphore_signal(barrier, inc=1, device_id={"tp": peer}, device_id_type=MESH)
    for other in other_grps:
        pl.semaphore_signal(barrier, inc=1, device_id={"grp": other}, device_id_type=MESH)

    @pl.when(f > 0)
    def _():
        pl.semaphore_signal(barrier, inc=1, device_id={"fs": f - 1}, device_id_type=MESH)

    @pl.when(f < planes - 1)
    def _():
        pl.semaphore_signal(barrier, inc=1, device_id={"fs": f + 1}, device_id_type=MESH)

    inner = jnp.where(f > 0, 1, 0) + jnp.where(f < planes - 1, 1, 0)
    pl.semaphore_wait(barrier, len(peers) + len(other_grps) + inner)

    def value_copy(phase, peer, slot):
        ref = input_all if phase == 0 else value_all.at[phase - 1]
        return pltpu.make_async_remote_copy(
            src_ref=payload if phase == 0 else ref.at[tp],
            dst_ref=ref.at[slot],
            send_sem=x_send.at[phase, peer],
            recv_sem=x_recv.at[phase, slot],
            device_id={"tp": peer},
            device_id_type=MESH,
        )

    def sum_copy(phase, peer, slot):
        return pltpu.make_async_remote_copy(
            src_ref=parts.at[phase, peer],
            dst_ref=sums.at[phase, slot],
            send_sem=s_send.at[phase, peer],
            recv_sem=s_recv.at[phase, slot],
            device_id={"tp": peer},
            device_id_type=MESH,
        )

    weights = (
        (gate_w, gate_all, False),
        (up_w, up_all, False),
        (down_w, down_all, True),
        (pool_w, pool_all, False),
        (mgate_w, mgate_all, False),
        (mout_w, mout_all, True),
    )
    pieces = []
    for number, (shard, whole, stacked) in enumerate(weights):
        for part in range(piece_counts[number]):
            pieces.append((number, part))

    def place(piece, plane, grp):
        number, part = pieces[piece]
        shard, whole, stacked = weights[number]
        tall = shard.shape[0]
        half = tall // grps
        size = half // piece_counts[number]
        start = grp * half + part * size
        if stacked:
            return whole.at[plane, pl.ds(pl.multiple_of(start, 16), size), :]
        return whole.at[pl.ds(pl.multiple_of(plane * tall + start, 16), size), :]

    def own_place(piece):
        number, part = pieces[piece]
        shard = weights[number][0]
        half = shard.shape[0] // grps
        size = half // piece_counts[number]
        return shard.at[pl.ds(pl.multiple_of(g * half + part * size, 16), size), :]

    def z_copy(piece, plane, step, own=False):
        spot = place(piece, plane, g)
        return pltpu.make_async_remote_copy(
            src_ref=own_place(piece) if own else spot,
            dst_ref=spot,
            send_sem=(up_sem if step > 0 else low_sem).at[piece, plane],
            recv_sem=z_recv.at[piece, plane],
            device_id={"fs": f + step},
            device_id_type=MESH,
        )

    def y_copy(piece, plane, number, source):
        spot = place(piece, plane, source)
        return pltpu.make_async_remote_copy(
            src_ref=spot,
            dst_ref=spot,
            send_sem=y_sem.at[piece, plane, number],
            recv_sem=y_recv.at[piece, plane, source],
            device_id={"grp": other_grps[number]},
            device_id_type=MESH,
        )

    def send_own(piece):
        if piece >= len(pieces):
            return

        @pl.when(f < planes - 1)
        def _():
            z_copy(piece, f, 1, own=True).start()

        @pl.when(f > 0)
        def _():
            z_copy(piece, f, -1, own=True).start()

    def pass_on(piece):
        send_own(piece + 2)
        for hop in range(1, planes):

            @pl.when(f >= hop)
            def _():
                z_copy(piece, f - hop, -1).wait_recv()

                @pl.when(f < planes - 1)
                def _():
                    z_copy(piece, f - hop, 1).start()

                for number in range(len(other_grps)):
                    y_copy(piece, f - hop, number, g).start()

            @pl.when(f + hop < planes)
            def _():
                z_copy(piece, f + hop, 1).wait_recv()

                @pl.when(f > 0)
                def _():
                    z_copy(piece, f + hop, -1).start()

                for number in range(len(other_grps)):
                    y_copy(piece, f + hop, number, g).start()

    def of(*numbers):
        return [p for p, (number, part) in enumerate(pieces) if number in numbers]

    def arrive(*numbers):
        for number in numbers:
            shard, whole, stacked = weights[number]
            local_copy(number).wait()
        for piece in of(*numbers):
            for step in range(1, planes):
                plane = (f + step) % planes
                for number, other in enumerate(other_grps):
                    y_copy(piece, plane, number, other).wait_recv()

    def local_copy(number):
        shard, whole, stacked = weights[number]
        tall = shard.shape[0]
        spot = whole.at[f] if stacked else whole.at[pl.ds(pl.multiple_of(f * tall, 16), tall), :]
        return pltpu.make_async_copy(shard, spot, local_sem.at[number])

    def local_input():
        return pltpu.make_async_copy(payload, input_all.at[tp], local_sem.at[len(weights)])

    row_tile = 32

    def scale_values(phase):
        for peer in peers:
            value_copy(phase, peer, peer).wait_recv()
        ref = input_all if phase == 0 else value_all.at[phase - 1]

        def body(step, carry):
            span = pl.ds(pl.multiple_of(step * row_tile, row_tile), row_tile)
            total = jnp.zeros((row_tile, 1), F32)
            for t in range(tps):
                gains = input_all[t, rows : rows + GAIN_ROWS, :].astype(F32)
                value = ref[t, span, :].astype(F32)
                total = total + jnp.sum(value * value, axis=1, keepdims=True)
                scaled[span, t * width : (t + 1) * width] = (
                    value * gains[phase : phase + 1]
                ).astype(BF16)
            factor[span, :] = lax.rsqrt(total / (tps * width) + 1e-06)
            return carry

        lax.fori_loop(0, rows // row_tile, body, 0)

    def hidden_units():
        units = hidden.shape[1]
        tile = 256 if units % 256 == 0 else 128

        def body(step, carry):
            span = pl.ds(pl.multiple_of(step * tile, tile), tile)
            gate = factor[...] * jnp.dot(
                scaled[...], gate_all[:, span], preferred_element_type=F32
            )
            up = factor[...] * jnp.dot(scaled[...], up_all[:, span], preferred_element_type=F32)
            hidden[:, span] = (jax.nn.silu(gate) * up).astype(BF16)
            return carry

        lax.fori_loop(0, units // tile, body, 0)

    def project(phase, left, right_all):
        ratio = planes // tps
        block = right_all.shape[2]
        for peer in peers + [tp]:
            for piece in range(ratio):
                parts[phase, peer, :, piece * block : (piece + 1) * block] = jnp.dot(
                    left[...], right_all[peer * ratio + piece], preferred_element_type=F32
                ).astype(BF16)
            if peer is not tp:
                sum_copy(phase, peer, tp).start()

    def total_of(phase):
        for peer in peers:
            sum_copy(phase, peer, peer).wait_recv()
        total = parts[phase, tp].astype(F32)
        for peer in peers:
            total = total + sums[phase, peer].astype(F32)
        return total

    def spread(phase):
        for peer in peers:
            value_copy(phase, peer, tp).start()

    local_input().start()
    spread(0)
    send_own(0)
    send_own(1)
    for number in range(len(weights)):
        local_copy(number).start()
    first_pieces = of(0, 1)
    pass_on(first_pieces[0])
    local_input().wait()
    scale_values(0)
    for piece in first_pieces[1:]:
        pass_on(piece)
    for piece in of(2)[:1]:
        pass_on(piece)
    arrive(0, 1)
    hidden_units()
    for piece in of(2)[1:]:
        pass_on(piece)
    arrive(2)
    project(0, hidden, down_all)

    for piece in of(3):
        pass_on(piece)
    value_all[0, tp] = (
        input_all[tp, 0:rows, :].astype(F32) + 0.5 * total_of(0)
    ).astype(BF16)
    spread(1)
    for piece in of(4):
        pass_on(piece)
    scale_values(1)
    for piece in of(5):
        pass_on(piece)
    arrive(3, 4)
    groups, group_width = mix_w.shape[0], mix_w.shape[1]
    pool_pre = (
        factor[...] * jnp.dot(scaled[...], pool_all[...], preferred_element_type=F32)
    ).astype(BF16)
    position = lax.broadcasted_iota(jnp.int32, (rows, group_width), 0)
    for group in range(groups):
        span = slice(group * group_width, (group + 1) * group_width)
        value = pool_pre[:, span].astype(F32)
        kind = (tp * groups + group) % 4
        running = value
        chosen = jnp.zeros_like(value)
        for level in range(4):
            lag = 2**level
            running = running + jnp.where(
                position >= lag, pltpu.roll(running, lag, axis=0), 0.0
            )
            counts = jnp.minimum(position + 1, 2 * lag).astype(F32)
            chosen = jnp.where(kind == level, running / counts, chosen)
        trail = (chosen - value).astype(BF16)
        mixed = jnp.dot(trail, mix_w[group], preferred_element_type=F32)
        pooled[:, span] = (mixed * scale_w[:, span]).astype(BF16)
    arrive(5)
    project(1, pooled, mout_all)
    logit[...] = factor[...] * jnp.dot(scaled[...], mgate_all[...], preferred_element_type=F32)
    value_all[1, tp] = (
        value_all[0, tp].astype(F32) + jax.nn.sigmoid(logit[...]) * total_of(1)
    ).astype(BF16)

    spread(2)
    scale_values(2)
    hidden_units()
    project(2, hidden, down_all)
    out[...] = (value_all[1, tp].astype(F32) + 0.5 * total_of(2)).astype(BF16)

    for phase in range(3):
        for peer in peers:
            value_copy(phase, peer, tp).wait_send()
            sum_copy(phase, peer, tp).wait_send()
    for piece in range(len(pieces)):

        @pl.when(f < planes - 1)
        def _():
            z_copy(piece, f, 1, own=True).wait_send()

        @pl.when(f > 0)
        def _():
            z_copy(piece, f, -1, own=True).wait_send()

        for hop in range(1, planes):

            @pl.when(f >= hop)
            def _():
                @pl.when(f < planes - 1)
                def _():
                    z_copy(piece, f - hop, 1).wait_send()

                for number in range(len(other_grps)):
                    y_copy(piece, f - hop, number, g).wait_send()

            @pl.when(f + hop < planes)
            def _():
                @pl.when(f > 0)
                def _():
                    z_copy(piece, f + hop, -1).wait_send()

                for number in range(len(other_grps)):
                    y_copy(piece, f + hop, number, g).wait_send()


def per_device(
    grps,
    planes,
    tps,
    layer_input,
    first_gain,
    ffn_gate_w,
    ffn_up_w,
    ffn_down_w,
    mixer_gain,
    pool_in_w,
    mixer_gate_w,
    group_mix_w,
    pool_scale,
    mixer_out_w,
    second_gain,
):
    rows, width = layer_input.shape
    features = width * tps
    gains = jnp.concatenate([first_gain, mixer_gain, second_gain], axis=0)
    payload = jnp.concatenate(
        [layer_input, jnp.pad(gains, ((0, GAIN_ROWS - 3), (0, 0)))], axis=0
    )
    units = ffn_gate_w.shape[1]
    channels = pool_in_w.shape[1]
    wanted = (2, 2, 2, 1, 1, 1)
    shards = (ffn_gate_w, ffn_up_w, ffn_down_w, pool_in_w, mixer_gate_w, mixer_out_w)
    piece_counts = tuple(
        ceil_pieces(shard.shape[0] // grps, count) for shard, count in zip(shards, wanted)
    )
    n = sum(piece_counts)
    dma = pltpu.SemaphoreType.DMA
    whole = pl.BlockSpec(memory_space=pltpu.VMEM)
    remote = pl.BlockSpec(memory_space=pl.ANY)
    return pl.pallas_call(
        functools.partial(layer_kernel, (grps, planes, tps, piece_counts)),
        out_shape=jax.ShapeDtypeStruct((rows, width), BF16),
        in_specs=[remote] * 7 + [whole] * 2,
        out_specs=whole,
        scratch_shapes=[
            pltpu.VMEM((features, units), BF16),
            pltpu.VMEM((features, units), BF16),
            pltpu.VMEM((planes,) + ffn_down_w.shape, BF16),
            pltpu.VMEM((features, channels), BF16),
            pltpu.VMEM((features, width), BF16),
            pltpu.VMEM((planes,) + mixer_out_w.shape, BF16),
            pltpu.VMEM((tps, rows + GAIN_ROWS, width), BF16),
            pltpu.VMEM((2, tps, rows, width), BF16),
            pltpu.VMEM((rows, features), BF16),
            pltpu.VMEM((rows, 1), F32),
            pltpu.VMEM((rows, units), BF16),
            pltpu.VMEM((rows, channels), BF16),
            pltpu.VMEM((rows, width), F32),
            pltpu.VMEM((3, tps, rows, width), BF16),
            pltpu.VMEM((3, tps, rows, width), BF16),
            dma((len(shards) + 1,)),
            dma((n, planes)),
            dma((n, planes, grps)),
            dma((n, planes)),
            dma((n, planes)),
            dma((n, planes, max(grps - 1, 1))),
            dma((3, tps)),
            dma((3, tps)),
            dma((3, tps)),
            dma((3, tps)),
        ],
        compiler_params=pltpu.CompilerParams(
            collective_id=0, has_side_effects=True, vmem_limit_bytes=60 * 1024 * 1024
        ),
    )(payload, *shards, group_mix_w, pool_scale)


def solution(mesh):
    return jax.shard_map(
        functools.partial(
            per_device, mesh.shape["grp"], mesh.shape["fs"], mesh.shape["tp"]
        ),
        mesh=mesh,
        in_specs=(
            P(("grp", "fs"), "tp"),
            P(None, "tp"),
            P("fs", "tp"),
            P("fs", "tp"),
            P("tp", "fs"),
            P(None, "tp"),
            P("fs", "tp"),
            P("fs", "tp"),
            P("tp", None, None),
            P(None, "tp"),
            P("tp", "fs"),
            P(None, "tp"),
        ),
        out_specs=P(("grp", "fs"), "tp"),
        check_vma=False,
    )
```

```python
import functools

import jax
import jax.numpy as jnp
from jax import lax
from jax.experimental import pallas as pl
from jax.experimental.pallas import tpu as pltpu
from jax.sharding import PartitionSpec as P

MESH = pl.DeviceIdType.MESH
F32 = jnp.float32
BF16 = jnp.bfloat16
GAIN_ROWS = 16


def ceil_pieces(rows, wanted):
    while rows % (wanted * 16) != 0:
        wanted -= 1
    return wanted


def layer_kernel(
    sizes,
    payload,
    gate_w,
    up_w,
    down_w,
    pool_w,
    mgate_w,
    mout_w,
    mix_w,
    scale_w,
    out,
    gate_all,
    up_all,
    down_all,
    pool_all,
    mgate_all,
    mout_all,
    input_all,
    value_all,
    scaled,
    factor,
    hidden,
    pooled,
    logit,
    parts,
    sums,
    local_sem,
    z_recv,
    y_recv,
    up_sem,
    low_sem,
    y_sem,
    x_send,
    x_relay,
    x_recv,
    s_send,
    s_recv,
):
    grps, planes, tps, piece_counts = sizes
    g = lax.axis_index("grp")
    f = lax.axis_index("fs")
    tp = lax.axis_index("tp")
    rows, width = out.shape
    chips = tps // 2
    chip, core = tp // 2, tp % 2
    partner = chip * 2 + (core + 1) % 2
    twins = [((chip + i) % chips) * 2 + core for i in range(1, chips)]
    crosses = [((chip + i) % chips) * 2 + (core + 1) % 2 for i in range(1, chips)]
    peers = twins + [partner]
    other_grps = [(g + d) % grps for d in range(1, grps)]

    barrier = pltpu.get_barrier_semaphore()
    for peer in peers:
        pl.semaphore_signal(barrier, inc=1, device_id={"tp": peer}, device_id_type=MESH)
    for other in other_grps:
        pl.semaphore_signal(barrier, inc=1, device_id={"grp": other}, device_id_type=MESH)

    @pl.when(f > 0)
    def _():
        pl.semaphore_signal(barrier, inc=1, device_id={"fs": f - 1}, device_id_type=MESH)

    @pl.when(f < planes - 1)
    def _():
        pl.semaphore_signal(barrier, inc=1, device_id={"fs": f + 1}, device_id_type=MESH)

    inner = jnp.where(f > 0, 1, 0) + jnp.where(f < planes - 1, 1, 0)
    pl.semaphore_wait(barrier, len(peers) + len(other_grps) + inner)

    def value_copy(phase, block, peer, relay=False):
        ref = input_all if phase == 0 else value_all.at[phase - 1]
        fresh = phase == 0 and not relay
        return pltpu.make_async_remote_copy(
            src_ref=payload if fresh else ref.at[block],
            dst_ref=ref.at[block],
            send_sem=x_relay.at[phase, block] if relay else x_send.at[phase, peer],
            recv_sem=x_recv.at[phase, block],
            device_id={"tp": peer},
            device_id_type=MESH,
        )

    def sum_copy(phase, block, slot, peer):
        return pltpu.make_async_remote_copy(
            src_ref=parts.at[phase, block],
            dst_ref=sums.at[phase, slot],
            send_sem=s_send.at[phase, block],
            recv_sem=s_recv.at[phase, slot],
            device_id={"tp": peer},
            device_id_type=MESH,
        )

    weights = (
        (gate_w, gate_all, False),
        (up_w, up_all, False),
        (down_w, down_all, True),
        (pool_w, pool_all, False),
        (mgate_w, mgate_all, False),
        (mout_w, mout_all, True),
    )
    pieces = []
    for number, (shard, whole, stacked) in enumerate(weights):
        for part in range(piece_counts[number]):
            pieces.append((number, part))

    def place(piece, plane, grp):
        number, part = pieces[piece]
        shard, whole, stacked = weights[number]
        tall = shard.shape[0]
        half = tall // grps
        size = half // piece_counts[number]
        start = grp * half + part * size
        if stacked:
            return whole.at[plane, pl.ds(pl.multiple_of(start, 16), size), :]
        return whole.at[pl.ds(pl.multiple_of(plane * tall + start, 16), size), :]

    def own_place(piece):
        number, part = pieces[piece]
        shard = weights[number][0]
        half = shard.shape[0] // grps
        size = half // piece_counts[number]
        return shard.at[pl.ds(pl.multiple_of(g * half + part * size, 16), size), :]

    def z_copy(piece, plane, step, own=False):
        spot = place(piece, plane, g)
        return pltpu.make_async_remote_copy(
            src_ref=own_place(piece) if own else spot,
            dst_ref=spot,
            send_sem=(up_sem if step > 0 else low_sem).at[piece, plane],
            recv_sem=z_recv.at[piece, plane],
            device_id={"fs": f + step},
            device_id_type=MESH,
        )

    def y_copy(piece, plane, number, source):
        spot = place(piece, plane, source)
        return pltpu.make_async_remote_copy(
            src_ref=spot,
            dst_ref=spot,
            send_sem=y_sem.at[piece, plane, number],
            recv_sem=y_recv.at[piece, plane, source],
            device_id={"grp": other_grps[number]},
            device_id_type=MESH,
        )

    def send_own(piece):

        @pl.when(f < planes - 1)
        def _():
            z_copy(piece, f, 1, own=True).start()

        @pl.when(f > 0)
        def _():
            z_copy(piece, f, -1, own=True).start()

    def pass_on(piece):
        if piece + 1 < mixer_start:
            send_own(piece + 1)
        for hop in range(1, planes):

            @pl.when(f >= hop)
            def _():
                z_copy(piece, f - hop, -1).wait_recv()

                @pl.when(f < planes - 1)
                def _():
                    z_copy(piece, f - hop, 1).start()

                for number in range(len(other_grps)):
                    y_copy(piece, f - hop, number, g).start()

            @pl.when(f + hop < planes)
            def _():
                z_copy(piece, f + hop, 1).wait_recv()

                @pl.when(f > 0)
                def _():
                    z_copy(piece, f + hop, -1).start()

                for number in range(len(other_grps)):
                    y_copy(piece, f + hop, number, g).start()

    def of(*numbers):
        return [p for p, (number, part) in enumerate(pieces) if number in numbers]

    mixer_start = of(3)[0]

    def arrive(*numbers):
        for number in numbers:
            shard, whole, stacked = weights[number]
            local_copy(number).wait()
        for piece in of(*numbers):
            for step in range(1, planes):
                plane = (f + step) % planes
                for number, other in enumerate(other_grps):
                    y_copy(piece, plane, number, other).wait_recv()

    def local_copy(number):
        shard, whole, stacked = weights[number]
        tall = shard.shape[0]
        spot = whole.at[f] if stacked else whole.at[pl.ds(pl.multiple_of(f * tall, 16), tall), :]
        return pltpu.make_async_copy(shard, spot, local_sem.at[number])

    def local_input():
        return pltpu.make_async_copy(payload, input_all.at[tp], local_sem.at[len(weights)])

    row_tile = 32

    def scale_values(phase):
        for twin in twins:
            value_copy(phase, twin, partner).wait_recv()
            value_copy(phase, twin, partner, relay=True).start()
        for block in [partner] + crosses:
            value_copy(phase, block, partner).wait_recv()
        ref = input_all if phase == 0 else value_all.at[phase - 1]

        def body(step, carry):
            span = pl.ds(pl.multiple_of(step * row_tile, row_tile), row_tile)
            total = jnp.zeros((row_tile, 1), F32)
            for t in range(tps):
                gains = input_all[t, rows : rows + GAIN_ROWS, :].astype(F32)
                value = ref[t, span, :].astype(F32)
                total = total + jnp.sum(value * value, axis=1, keepdims=True)
                scaled[span, t * width : (t + 1) * width] = (
                    value * gains[phase : phase + 1]
                ).astype(BF16)
            factor[span, :] = lax.rsqrt(total / (tps * width) + 1e-06)
            return carry

        lax.fori_loop(0, rows // row_tile, body, 0)

    def hidden_units():
        units = hidden.shape[1]
        tile = 256 if units % 256 == 0 else 128

        def body(step, carry):
            span = pl.ds(pl.multiple_of(step * tile, tile), tile)
            gate = factor[...] * jnp.dot(
                scaled[...], gate_all[:, span], preferred_element_type=F32
            )
            up = factor[...] * jnp.dot(scaled[...], up_all[:, span], preferred_element_type=F32)
            hidden[:, span] = (jax.nn.silu(gate) * up).astype(BF16)
            return carry

        lax.fori_loop(0, units // tile, body, 0)

    def project(phase, left, right_all):
        ratio = planes // tps
        block = right_all.shape[2]

        def compute(block_of):
            for piece in range(ratio):
                parts[phase, block_of, :, piece * block : (piece + 1) * block] = jnp.dot(
                    left[...], right_all[block_of * ratio + piece], preferred_element_type=F32
                ).astype(BF16)

        for twin, cross in zip(twins, crosses):
            compute(cross)
            sum_copy(phase, cross, twin, partner).start()
        for twin, cross in zip(twins, crosses):
            compute(twin)
            sum_copy(phase, cross, cross, partner).wait_recv()
            parts[phase, twin] = (
                parts[phase, twin].astype(F32) + sums[phase, cross].astype(F32)
            ).astype(BF16)
            sum_copy(phase, twin, tp, twin).start()
        compute(partner)
        sum_copy(phase, partner, tp, partner).start()
        compute(tp)

    def total_of(phase):
        total = parts[phase, tp].astype(F32)
        for peer in [partner] + twins:
            sum_copy(phase, peer, peer, partner).wait_recv()
            total = total + sums[phase, peer].astype(F32)
        return total

    def spread(phase):
        for peer in peers:
            value_copy(phase, tp, peer).start()

    local_input().start()
    spread(0)
    send_own(0)
    for number in range(len(weights)):
        local_copy(number).start()
    first_pieces = of(0, 1)
    pass_on(first_pieces[0])
    local_input().wait()
    scale_values(0)
    for piece in first_pieces[1:]:
        pass_on(piece)
    for piece in of(2)[:1]:
        pass_on(piece)
    arrive(0, 1)
    hidden_units()
    for piece in of(2)[1:]:
        pass_on(piece)
    for piece in range(mixer_start, len(pieces)):
        send_own(piece)
    arrive(2)
    project(0, hidden, down_all)

    for piece in of(3):
        pass_on(piece)
    value_all[0, tp] = (
        input_all[tp, 0:rows, :].astype(F32) + 0.5 * total_of(0)
    ).astype(BF16)
    spread(1)
    for piece in of(4):
        pass_on(piece)
    scale_values(1)
    for piece in of(5):
        pass_on(piece)
    arrive(3, 4)
    groups, group_width = mix_w.shape[0], mix_w.shape[1]
    pool_pre = (
        factor[...] * jnp.dot(scaled[...], pool_all[...], preferred_element_type=F32)
    ).astype(BF16)
    position = lax.broadcasted_iota(jnp.int32, (rows, group_width), 0)
    for group in range(groups):
        span = slice(group * group_width, (group + 1) * group_width)
        value = pool_pre[:, span].astype(F32)
        kind = (tp * groups + group) % 4
        running = value
        chosen = jnp.zeros_like(value)
        for level in range(4):
            lag = 2**level
            running = running + jnp.where(
                position >= lag, pltpu.roll(running, lag, axis=0), 0.0
            )
            counts = jnp.minimum(position + 1, 2 * lag).astype(F32)
            chosen = jnp.where(kind == level, running / counts, chosen)
        trail = (chosen - value).astype(BF16)
        mixed = jnp.dot(trail, mix_w[group], preferred_element_type=F32)
        pooled[:, span] = (mixed * scale_w[:, span]).astype(BF16)
    arrive(5)
    project(1, pooled, mout_all)
    logit[...] = factor[...] * jnp.dot(scaled[...], mgate_all[...], preferred_element_type=F32)
    value_all[1, tp] = (
        value_all[0, tp].astype(F32) + jax.nn.sigmoid(logit[...]) * total_of(1)
    ).astype(BF16)

    spread(2)
    scale_values(2)
    hidden_units()
    project(2, hidden, down_all)
    out[...] = (value_all[1, tp].astype(F32) + 0.5 * total_of(2)).astype(BF16)

    for phase in range(3):
        for peer in peers:
            value_copy(phase, tp, peer).wait_send()
        for twin in twins:
            value_copy(phase, twin, partner, relay=True).wait_send()
        for block in crosses + twins + [partner]:
            sum_copy(phase, block, tp, partner).wait_send()
    for piece in range(len(pieces)):

        @pl.when(f < planes - 1)
        def _():
            z_copy(piece, f, 1, own=True).wait_send()

        @pl.when(f > 0)
        def _():
            z_copy(piece, f, -1, own=True).wait_send()

        for hop in range(1, planes):

            @pl.when(f >= hop)
            def _():
                @pl.when(f < planes - 1)
                def _():
                    z_copy(piece, f - hop, 1).wait_send()

                for number in range(len(other_grps)):
                    y_copy(piece, f - hop, number, g).wait_send()

            @pl.when(f + hop < planes)
            def _():
                @pl.when(f > 0)
                def _():
                    z_copy(piece, f + hop, -1).wait_send()

                for number in range(len(other_grps)):
                    y_copy(piece, f + hop, number, g).wait_send()


def per_device(
    grps,
    planes,
    tps,
    layer_input,
    first_gain,
    ffn_gate_w,
    ffn_up_w,
    ffn_down_w,
    mixer_gain,
    pool_in_w,
    mixer_gate_w,
    group_mix_w,
    pool_scale,
    mixer_out_w,
    second_gain,
):
    rows, width = layer_input.shape
    features = width * tps
    gains = jnp.concatenate([first_gain, mixer_gain, second_gain], axis=0)
    payload = jnp.concatenate(
        [layer_input, jnp.pad(gains, ((0, GAIN_ROWS - 3), (0, 0)))], axis=0
    )
    units = ffn_gate_w.shape[1]
    channels = pool_in_w.shape[1]
    fine = max(16 // planes, 1)
    wanted = (fine, fine, fine, max(fine // 4, 1), max(fine // 2, 1), max(fine // 4, 1))
    shards = (ffn_gate_w, ffn_up_w, ffn_down_w, pool_in_w, mixer_gate_w, mixer_out_w)
    piece_counts = tuple(
        ceil_pieces(shard.shape[0] // grps, count) for shard, count in zip(shards, wanted)
    )
    n = sum(piece_counts)
    dma = pltpu.SemaphoreType.DMA
    whole = pl.BlockSpec(memory_space=pltpu.VMEM)
    remote = pl.BlockSpec(memory_space=pl.ANY)
    return pl.pallas_call(
        functools.partial(layer_kernel, (grps, planes, tps, piece_counts)),
        out_shape=jax.ShapeDtypeStruct((rows, width), BF16),
        in_specs=[remote] * 7 + [whole] * 2,
        out_specs=whole,
        scratch_shapes=[
            pltpu.VMEM((features, units), BF16),
            pltpu.VMEM((features, units), BF16),
            pltpu.VMEM((planes,) + ffn_down_w.shape, BF16),
            pltpu.VMEM((features, channels), BF16),
            pltpu.VMEM((features, width), BF16),
            pltpu.VMEM((planes,) + mixer_out_w.shape, BF16),
            pltpu.VMEM((tps, rows + GAIN_ROWS, width), BF16),
            pltpu.VMEM((2, tps, rows, width), BF16),
            pltpu.VMEM((rows, features), BF16),
            pltpu.VMEM((rows, 1), F32),
            pltpu.VMEM((rows, units), BF16),
            pltpu.VMEM((rows, channels), BF16),
            pltpu.VMEM((rows, width), F32),
            pltpu.VMEM((3, tps, rows, width), BF16),
            pltpu.VMEM((3, tps, rows, width), BF16),
            dma((len(shards) + 1,)),
            dma((n, planes)),
            dma((n, planes, grps)),
            dma((n, planes)),
            dma((n, planes)),
            dma((n, planes, max(grps - 1, 1))),
            dma((3, tps)),
            dma((3, tps)),
            dma((3, tps)),
            dma((3, tps)),
            dma((3, tps)),
        ],
        compiler_params=pltpu.CompilerParams(
            collective_id=0, has_side_effects=True, vmem_limit_bytes=60 * 1024 * 1024
        ),
    )(payload, *shards, group_mix_w, pool_scale)


def solution(mesh):
    return jax.shard_map(
        functools.partial(
            per_device, mesh.shape["grp"], mesh.shape["fs"], mesh.shape["tp"]
        ),
        mesh=mesh,
        in_specs=(
            P(("grp", "fs"), "tp"),
            P(None, "tp"),
            P("fs", "tp"),
            P("fs", "tp"),
            P("tp", "fs"),
            P(None, "tp"),
            P("fs", "tp"),
            P("fs", "tp"),
            P("tp", None, None),
            P(None, "tp"),
            P("tp", "fs"),
            P(None, "tp"),
        ),
        out_specs=P(("grp", "fs"), "tp"),
        check_vma=False,
    )
```
